32 devices in a mesh: gr: 2 (over x), fs: 8 (over z, y), tp: 2 (over core).
Axes of the slice: x: 2, y: 2, z: 4, core: 2. Of those that a mesh axis runs over, the one named last changes fastest.
Arguments:
- prompt_tokens: bfloat16 [4608, 2048], P(('gr', 'fs', 'tp')), may hold values from -6 to 6
- up_master: float32 [2048, 8192], P(('gr', 'fs'), 'tp'), may hold values from -0.125 to 0.125
- down_master: float32 [2048, 8192], P(('gr', 'fs'), 'tp'), may hold values from -0.0625 to 0.0625
- norm_gain: float32 [2048], P(('gr', 'fs')), may hold values from 0.1 to 1.9
Outputs:
- sampler_up: bfloat16 [2048, 8192], P(None, ('gr', 'tp'))
- sampler_down: bfloat16 [2048, 8192], P(None, ('gr', 'tp'))
- prompt_out: bfloat16 [4608, 2048], P(('gr', 'fs', 'tp'))
The draws below stay inside these ranges and needn't reach their ends.
All inputs are finite; a program needn't handle non-finite values.
Results may differ from the reference program's by a relative error of at most 0.009.
Values may be sent and summed in bfloat16 or wider, within the bound.
A program may use at most 128 MiB of HBM per device.

```python
import jax
import jax.numpy as jnp
from jax import lax

D = 2048
FF = 8192
TOKENS = 4608
N_GR = 2
N_TP = 2


def steps_of(stream_key, dims, shards, low, high):
    level = 1.0
    for dim, parts in shards:
        draws = jax.random.uniform(jax.random.fold_in(jax.random.fold_in(stream_key, 6), dim), (parts,), jnp.float32, low / len(shards), high / len(shards))
        level = level * jnp.repeat(jnp.exp(draws), dims[dim] // parts).reshape((-1,) + (1,) * (len(dims) - 1 - dim))
    return level


def gaussian(own_key, shape, scale, reach, split=(), kind=jnp.bfloat16):
    drawn = jax.random.normal(own_key, shape, jnp.float32) * scale
    if len(split) > 0:
        drawn = steps_of(own_key, shape, split, -0.22, 0.18) * drawn
    return jnp.clip(drawn, min=-reach, max=reach).astype(kind)


def setup_inputs(seed: int = 0) -> dict:
    streams_of = jax.random.split(jax.random.key(seed), 5)
    prompt_tokens = gaussian(streams_of[0], (TOKENS, D), 1.0, 6.0, ((0, 32),))
    up_master = gaussian(streams_of[1], (D, FF), D ** -0.5, 0.125, ((0, 16), (1, 2)), jnp.float32)
    down_master = gaussian(streams_of[2], (D, FF), FF ** -0.5, 0.0625, ((0, 16), (1, 2)), jnp.float32)
    norm_gain = jnp.clip(1.0 + 0.18 * jax.random.normal(streams_of[3], (D,), jnp.float32), 0.1, 1.9)
    return {"prompt_tokens": prompt_tokens, "up_master": up_master, "down_master": down_master, "norm_gain": norm_gain}


def reference(prompt_tokens, up_master, down_master, norm_gain):
    sampler_up = (norm_gain[:, None] * up_master).astype(jnp.bfloat16)
    sampler_down = down_master.astype(jnp.bfloat16)
    values = prompt_tokens.astype(jnp.float32)
    center = lax.optimization_barrier(jnp.mean(values, axis=-1, keepdims=True))
    spread = lax.optimization_barrier(jnp.mean(jnp.square(values - center), axis=-1, keepdims=True))
    normed = ((values - center) * lax.rsqrt(spread + 1e-05)).astype(jnp.bfloat16)
    width = FF // (N_GR * N_TP)

    def block_step(total, index):
        start = (index * width).astype(jnp.int32)
        up_block = lax.dynamic_slice_in_dim(sampler_up, start, width, 1)
        down_block = lax.dynamic_slice_in_dim(sampler_down, start, width, 1)
        lifted = jax.nn.relu(jnp.dot(normed, up_block, preferred_element_type=jnp.float32))
        hidden = (lifted * lifted).astype(jnp.bfloat16)
        partial_value = lax.dot_general(hidden, down_block, (((1,), (1,)), ((), ())), preferred_element_type=jnp.float32)
        partial_value = lax.optimization_barrier(partial_value.astype(jnp.bfloat16)).astype(jnp.float32)
        return (total + partial_value, None)
    total, unused = lax.scan(block_step, jnp.zeros((TOKENS, D), jnp.float32), jnp.arange(N_GR * N_TP, dtype=jnp.int32))
    return (sampler_up, sampler_down, total.astype(jnp.bfloat16))
```

```python
import functools

import jax
import jax.numpy as jnp
from jax import lax
from jax.experimental import pallas as pl
from jax.experimental.pallas import tpu as pltpu
from jax.sharding import PartitionSpec as P

MESH = pl.DeviceIdType.MESH
CHUNK = 32
TILE = 256
PAIR_FIRST = (1, 2)


def kernel(G, F, T, tok_in, up_in, down_in, up_out, down_out, out_ref,
           full, nrm, hid, stage, part,
           recv, sendl, sendr, sendy, send0, tok_recv, tok_send,
           part_recv, part_send, local_sem):
    gr, f, tp = lax.axis_index("gr"), lax.axis_index("fs"), lax.axis_index("tp")
    A = F // 2
    a, y = f // 2, f % 2
    mate = a * 2 + 1 - y
    R = up_in.shape[0]
    D = full.shape[1]
    W = full.shape[2]
    tok = tok_in.shape[0]
    CH = min(CHUNK, R)
    C = R // CH
    NQ = G * C
    K = G * T
    k = gr * T + tp
    weights = (up_in, down_in)

    def at_k(kk):
        return (kk // T, f, kk % T)

    barrier = pltpu.get_barrier_semaphore()
    for d in range(1, K):
        pl.semaphore_signal(barrier, inc=1, device_id=at_k((k + d) % K), device_id_type=MESH)
    pl.semaphore_signal(barrier, inc=1, device_id=(gr, mate, tp), device_id_type=MESH)

    for shift in (1, A - 1):
        near = lax.rem(a + shift, A) * 2 + y
        pl.semaphore_signal(barrier, inc=1, device_id=(gr, near, tp), device_id_type=MESH)
    pl.semaphore_wait(barrier, K + 2)

    def rows_of(origin, g, c):
        return pl.ds(pl.multiple_of(g * (F * R) + origin * R + c * CH, CH), CH)

    def hand(m, b, c, wait):
        kk = tp * G + b
        dg = kk // T
        q = ((gr - dg + G) % G) * C + c
        src = weights[m].at[pl.ds(c * CH, CH), pl.ds(b * W, W)]
        dst = full.at[m, rows_of(f, gr, c)]

        @pl.when(kk == k)
        def _():
            if not wait:
                pltpu.make_async_copy(src, dst, recv.at[m, f, q]).start()

        @pl.when(kk != k)
        def _():
            copy = pltpu.make_async_remote_copy(
                src_ref=src, dst_ref=dst, send_sem=send0.at[m, b, c], recv_sem=recv.at[m, f, q],
                device_id=at_k(kk), device_id_type=MESH)
            if wait:
                copy.wait_send()
            else:
                copy.start()

    def tokens(wait):
        own = nrm.at[pl.ds(pl.multiple_of(k * tok, 16), tok)]
        if not wait:
            pltpu.make_async_copy(tok_in, own, local_sem.at[0]).start()
        for d in range(1, K):
            copy = pltpu.make_async_remote_copy(
                src_ref=tok_in, dst_ref=own, send_sem=tok_send.at[d - 1], recv_sem=tok_recv.at[d - 1],
                device_id=at_k((k + d) % K), device_id_type=MESH)
            if wait:
                copy.wait_send()
            else:
                copy.start()

    for m in range(2):
        for c in range(C):
            for b in range(G):
                hand(m, b, c, False)
        if m == 0:
            tokens(False)

    def chunk(m, origin, q):
        return full.at[m, rows_of(origin, (gr + q // C) % G, q % C)]

    def send(m, origin, q, sems, target, wait):
        ref = chunk(m, origin, q)
        copy = pltpu.make_async_remote_copy(
            src_ref=ref, dst_ref=ref, send_sem=sems.at[m, origin, q], recv_sem=recv.at[m, origin, q],
            device_id=(gr, target, tp), device_id_type=MESH)
        if wait:
            copy.wait_send()
        else:
            copy.start()

    def arrived(m, origin, q):
        ref = chunk(m, origin, q)
        pltpu.make_async_copy(ref, ref, recv.at[m, origin, q]).wait()

    def left(m, origin, q, wait):
        @pl.when(a > 0)
        def _():
            send(m, origin, q, sendl, f - 2, wait)

    def right(m, origin, q, wait):
        @pl.when(a < A - 1)
        def _():
            send(m, origin, q, sendr, f + 2, wait)

    def loop(low, high, step):
        def go(i, carry):
            step(i)
            return carry
        if high > low:
            lax.fori_loop(low, high, go, 0)

    def own(m, wait=False):
        def step(q):
            if not wait:
                arrived(m, f, q)
            left(m, f, q, wait)
            right(m, f, q, wait)
            send(m, f, q, sendy, mate, wait)
        loop(0, NQ, step)

    def mated(m, wait=False):
        def step(q):
            if not wait:
                arrived(m, mate, q)
            left(m, mate, q, wait)
            right(m, mate, q, wait)
        loop(0, PAIR_FIRST[m], step)

    def line(m, s, wait=False):
        below, above = a - 1 - s, a + 1 + s

        def pass_on(origin_a, side, q, onward, across):
            origin = origin_a * 2 + side
            if not wait:
                arrived(m, origin, q)
            onward(m, origin, q, wait)
            if across:
                send(m, origin, q, sendy, mate, wait)

        def both(side, across):
            def step(q):
                @pl.when(below >= 0)
                def _():
                    pass_on(below, side, q, right, across)

                @pl.when(above < A)
                def _():
                    pass_on(above, side, q, left, across)
            return step

        pf = PAIR_FIRST[m]
        loop(0, pf, both(y, False))
        loop(pf, NQ, both(y, True))
        loop(0, pf, both(1 - y, False))

    def settle(m, origin_a):
        loop(PAIR_FIRST[m], NQ, lambda q: arrived(m, origin_a * 2 + 1 - y, q))

    own(0)
    mated(0)
    loop(0, A - 2, lambda s: line(0, s))
    own(1)
    line(0, A - 2)
    mated(1)
    line(1, 0)

    loop(0, A, lambda i: settle(0, i))
    up_copy = pltpu.make_async_copy(full.at[0], up_out, local_sem.at[1])
    up_copy.start()
    pltpu.make_async_copy(tok_in, nrm.at[pl.ds(pl.multiple_of(k * tok, 16), tok)], local_sem.at[0]).wait()
    for d in range(1, K):
        there = nrm.at[pl.ds(pl.multiple_of(((k - d + K) % K) * tok, 16), tok)]
        pltpu.make_async_copy(there, there, tok_recv.at[d - 1]).wait()

    tile = min(TILE, W)

    def lift(j):
        columns = pl.ds(pl.multiple_of(j * tile, tile), tile)
        lifted = jnp.maximum(jnp.dot(nrm[...], full[0, :, columns], preferred_element_type=jnp.float32), 0.0)
        hid[:, columns] = (lifted * lifted).astype(jnp.bfloat16)
    loop(0, W // tile, lift)

    def part_copy(d, block):
        target = (k + d) % K
        return pltpu.make_async_remote_copy(
            src_ref=stage.at[block, pl.ds(pl.multiple_of(target * tok, 16), tok)],
            dst_ref=part.at[d - 1, block],
            send_sem=part_send.at[d - 1, block], recv_sem=part_recv.at[d - 1, block],
            device_id=at_k(target), device_id_type=MESH)

    def lower(origin_a):
        settle(1, origin_a)

        def group(g):
            block = origin_a * G + g
            rows = pl.ds(pl.multiple_of(g * (F * R) + origin_a * (2 * R), 2 * R), 2 * R)
            pltpu.make_async_copy(full.at[1, rows], down_out.at[rows], local_sem.at[2 + block]).start()
            value = lax.dot_general(hid[...], full[1, rows, :], (((1,), (1,)), ((), ())),
                                    preferred_element_type=jnp.float32)
            stage[block] = value.astype(jnp.bfloat16)
            for d in range(1, K):
                part_copy(d, block).start()
        loop(0, G, group)

    def lower_ring(s):
        @pl.when(a - 1 - s >= 0)
        def _():
            lower(a - 1 - s)

        @pl.when(a + 1 + s < A)
        def _():
            lower(a + 1 + s)

    lower(a)

    def tail(s):
        line(1, s)
        lower_ring(s - 1)
    loop(1, A - 1, tail)
    lower_ring(A - 2)

    mine = pl.ds(pl.multiple_of(k * tok, 16), tok)
    for block in range(A * G):
        total = stage[block, mine].astype(jnp.float32)
        for d in range(1, K):
            there = part.at[d - 1, block]
            pltpu.make_async_copy(there, there, part_recv.at[d - 1, block]).wait()
            total += part[d - 1, block].astype(jnp.float32)
        begin = (block % G) * (F * R) + (block // G) * (2 * R)
        out_ref[:, begin:begin + 2 * R] = total.astype(jnp.bfloat16)

    up_copy.wait()

    def drain(block):
        rows = pl.ds(0, 2 * R)
        pltpu.make_async_copy(full.at[1, rows], down_out.at[rows], local_sem.at[2 + block]).wait()
        for d in range(1, K):
            part_copy(d, block).wait_send()
    loop(0, A * G, drain)
    tokens(True)
    for m in range(2):
        for c in range(C):
            for b in range(G):
                hand(m, b, c, True)
        own(m, True)
        mated(m, True)
        loop(0, A - 1, lambda s: line(m, s, True))


def body(G, F, T, prompt_tokens, up_master, down_master, norm_gain):
    up_local = (norm_gain[:, None] * up_master).astype(jnp.bfloat16)
    down_local = down_master.astype(jnp.bfloat16)
    values = prompt_tokens.astype(jnp.float32)
    center = jnp.mean(values, axis=-1, keepdims=True)
    variance = jnp.mean(jnp.square(values - center), axis=-1, keepdims=True)
    normed = ((values - center) * lax.rsqrt(variance + 1e-05)).astype(jnp.bfloat16)
    R, width = up_local.shape
    tok = normed.shape[0]
    D, W = R * G * F, width // G
    A, K = F // 2, G * T
    C = R // min(CHUNK, R)
    NQ = G * C
    bf16 = jnp.bfloat16
    any_space = pl.BlockSpec(memory_space=pl.ANY)
    dma = pltpu.SemaphoreType.DMA
    return pl.pallas_call(
        functools.partial(kernel, G, F, T),
        name="handoff",
        out_shape=(
            jax.ShapeDtypeStruct((D, W), bf16),
            jax.ShapeDtypeStruct((D, W), bf16),
            jax.ShapeDtypeStruct((tok, D), bf16),
        ),
        in_specs=[any_space] * 3,
        out_specs=(any_space, any_space, pl.BlockSpec(memory_space=pltpu.VMEM)),
        scratch_shapes=[
            pltpu.VMEM((2, D, W), bf16),
            pltpu.VMEM((K * tok, D), bf16),
            pltpu.VMEM((K * tok, W), bf16),
            pltpu.VMEM((A * G, K * tok, 2 * R), bf16),
            pltpu.VMEM((K - 1, A * G, tok, 2 * R), bf16),
            dma((2, F, NQ)), dma((2, F, NQ)), dma((2, F, NQ)), dma((2, F, NQ)),
            dma((2, G, C)), dma((K - 1,)), dma((K - 1,)),
            dma((K - 1, A * G)), dma((K - 1, A * G)), dma((2 + A * G,)),
        ],
        compiler_params=pltpu.CompilerParams(
            collective_id=0, has_side_effects=True, vmem_limit_bytes=56 * 1024 * 1024),
    )(normed, up_local, down_local)


def solution(mesh):
    placed = (
        P(("gr", "fs", "tp"), None),
        P(("gr", "fs"), "tp"),
        P(("gr", "fs"), "tp"),
        P(("gr", "fs")),
    )
    return jax.shard_map(
        functools.partial(body, mesh.shape["gr"], mesh.shape["fs"], mesh.shape["tp"]),
        mesh=mesh,
        in_specs=placed,
        out_specs=(P(None, ("gr", "tp")), P(None, ("gr", "tp")), P(("gr", "fs", "tp"), None)),
        check_vma=False,
    )
```

```python
import functools

import jax
import jax.numpy as jnp
from jax import lax
from jax.experimental import pallas as pl
from jax.experimental.pallas import tpu as pltpu
from jax.sharding import PartitionSpec as P

MESH = pl.DeviceIdType.MESH
CHUNK = 32
TILE = 256
PAIR_FIRST = (1, 2)


def kernel(G, F, T, tok_in, gain_in, up_in, down_in, up_full, down_full, out_ref,
           wide, narrow, raw, nrm, hid, stage, part,
           recv, sendl, sendr, sendy, send0, tok_recv, tok_send,
           part_recv, part_send, local_sem, load_sem):
    gr, f, tp = lax.axis_index("gr"), lax.axis_index("fs"), lax.axis_index("tp")
    full = (up_full, down_full)
    A = F // 2
    a, y = f // 2, f % 2
    mate = a * 2 + 1 - y
    R = up_in.shape[0]
    D, W = up_full.shape
    tok = tok_in.shape[0]
    CH = min(CHUNK, R)
    C = R // CH
    NQ = G * C
    K = G * T
    k = gr * T + tp
    weights = (up_in, down_in)

    def at_k(kk):
        return (kk // T, f, kk % T)

    def load(m, c):
        rows = pl.ds(c * CH, CH)
        return pltpu.make_async_copy(weights[m].at[rows], wide.at[m, rows], load_sem.at[m, c])

    token_load = pltpu.make_async_copy(tok_in, raw, local_sem.at[0])
    for c in range(C):
        load(0, c).start()
    token_load.start()
    for c in range(C):
        load(1, c).start()

    barrier = pltpu.get_barrier_semaphore()
    for d in range(1, K):
        pl.semaphore_signal(barrier, inc=1, device_id=at_k((k + d) % K), device_id_type=MESH)
    pl.semaphore_signal(barrier, inc=1, device_id=(gr, mate, tp), device_id_type=MESH)

    for shift in (1, A - 1):
        near = lax.rem(a + shift, A) * 2 + y
        pl.semaphore_signal(barrier, inc=1, device_id=(gr, near, tp), device_id_type=MESH)
    pl.semaphore_wait(barrier, K + 2)

    def rows_of(origin, g, c):
        return pl.ds(pl.multiple_of(g * (F * R) + origin * R + c * CH, CH), CH)

    home = k // G == tp

    def cast(m, c):
        rows = pl.ds(c * CH, CH)
        load(m, c).wait()
        value = wide[m, rows, :]
        if m == 0:
            value = value * column[c * CH:(c + 1) * CH]
        value = value.astype(jnp.bfloat16)
        narrow[m, rows, :] = value
        for b in range(G):
            @pl.when(tp * G + b == k)
            def _():
                full[m][rows_of(f, gr, c), :] = value[:, b * W:(b + 1) * W]

    def hand(m, b, c, wait):
        kk = tp * G + b
        q = ((gr - kk // T + G) % G) * C + c

        @pl.when(kk != k)
        def _():
            copy = pltpu.make_async_remote_copy(
                src_ref=narrow.at[m, pl.ds(c * CH, CH), pl.ds(b * W, W)],
                dst_ref=full[m].at[rows_of(f, gr, c)],
                send_sem=send0.at[m, b, c], recv_sem=recv.at[m, f, q],
                device_id=at_k(kk), device_id_type=MESH)
            if wait:
                copy.wait_send()
            else:
                copy.start()

    mine = pl.ds(pl.multiple_of(k * tok, 16), tok)

    def tokens(wait):
        for d in range(1, K):
            copy = pltpu.make_async_remote_copy(
                src_ref=nrm.at[mine], dst_ref=nrm.at[mine],
                send_sem=tok_send.at[d - 1], recv_sem=tok_recv.at[d - 1],
                device_id=at_k((k + d) % K), device_id_type=MESH)
            if wait:
                copy.wait_send()
            else:
                copy.start()

    def normalize(i, carry):
        values = raw[pl.ds(pl.multiple_of(i * 16, 16), 16), :].astype(jnp.float32)
        center = jnp.mean(values, axis=-1, keepdims=True)
        moved = values - center
        spread = jnp.mean(jnp.square(moved), axis=-1, keepdims=True)
        nrm[pl.ds(pl.multiple_of(k * tok + i * 16, 16), 16), :] = (
            moved * lax.rsqrt(spread + 1e-05)).astype(jnp.bfloat16)
        return carry

    rowed = lax.broadcasted_iota(jnp.int32, (R, R), 0) == lax.broadcasted_iota(jnp.int32, (R, R), 1)
    column = jnp.sum(jnp.where(rowed, gain_in[...], 0.0), axis=1, keepdims=True)

    cast(0, 0)
    for c in range(C):
        if c + 1 < C:
            cast(0, c + 1)
        else:
            cast(1, 0)
        for b in range(G):
            hand(0, b, c, False)

    def chunk(m, origin, q):
        return full[m].at[rows_of(origin, (gr + q // C) % G, q % C)]

    def send(m, origin, q, sems, target, wait):
        ref = chunk(m, origin, q)
        copy = pltpu.make_async_remote_copy(
            src_ref=ref, dst_ref=ref, send_sem=sems.at[m, origin, q], recv_sem=recv.at[m, origin, q],
            device_id=(gr, target, tp), device_id_type=MESH)
        if wait:
            copy.wait_send()
        else:
            copy.start()

    def arrived(m, origin, q):
        ref = chunk(m, origin, q)
        pltpu.make_async_copy(ref, ref, recv.at[m, origin, q]).wait()

    def left(m, origin, q, wait):
        @pl.when(a > 0)
        def _():
            send(m, origin, q, sendl, f - 2, wait)

    def right(m, origin, q, wait):
        @pl.when(a < A - 1)
        def _():
            send(m, origin, q, sendr, f + 2, wait)

    def loop(low, high, step):
        def go(i, carry):
            step(i)
            return carry
        if high > low:
            lax.fori_loop(low, high, go, 0)

    def own(m, wait=False):
        def step(q):
            if not wait:
                @pl.when(jnp.logical_or(q >= C, jnp.logical_not(home)))
                def _():
                    arrived(m, f, q)
            left(m, f, q, wait)
            right(m, f, q, wait)
            send(m, f, q, sendy, mate, wait)
        loop(0, NQ, step)

    def mated(m, wait=False):
        def step(q):
            if not wait:
                arrived(m, mate, q)
            left(m, mate, q, wait)
            right(m, mate, q, wait)
        loop(0, PAIR_FIRST[m], step)

    def line(m, s, wait=False, between=None):
        below, above = a - 1 - s, a + 1 + s

        def pass_on(origin_a, side, q, onward, across):
            origin = origin_a * 2 + side
            if not wait:
                arrived(m, origin, q)
            onward(m, origin, q, wait)
            if across:
                send(m, origin, q, sendy, mate, wait)

        def both(side, across):
            def step(q):
                @pl.when(below >= 0)
                def _():
                    pass_on(below, side, q, right, across)

                @pl.when(above < A)
                def _():
                    pass_on(above, side, q, left, across)
            return step

        pf = PAIR_FIRST[m]
        loop(0, pf, both(y, False))
        half = NQ // 2 + 1 if between is not None else NQ
        loop(pf, half, both(y, True))
        if between is not None:
            between()
        loop(half, NQ, both(y, True))
        loop(0, pf, both(1 - y, False))

    def settle(m, origin_a, gi):
        low = jnp.maximum(PAIR_FIRST[m], gi * C)

        def go(q, carry):
            arrived(m, origin_a * 2 + 1 - y, q)
            return carry
        lax.fori_loop(low, (gi + 1) * C, go, 0)

    def settle_all(i):
        for gi in range(G):
            settle(0, i, gi)

    own(0)
    token_load.wait()
    lax.fori_loop(0, tok // 16, normalize, 0)
    for c in range(C):
        if c + 1 < C:
            cast(1, c + 1)
        for b in range(G):
            hand(1, b, c, False)
    tokens(False)
    mated(0)
    loop(0, A - 2, lambda s: line(0, s))
    own(1)
    line(0, A - 2)
    mated(1)
    line(1, 0)

    loop(0, A, settle_all)
    for d in range(1, K):
        there = nrm.at[pl.ds(pl.multiple_of(((k - d + K) % K) * tok, 16), tok)]
        pltpu.make_async_copy(there, there, tok_recv.at[d - 1]).wait()

    tile = min(TILE, W)

    def lift(j):
        columns = pl.ds(pl.multiple_of(j * tile, tile), tile)
        lifted = jnp.maximum(jnp.dot(nrm[...], up_full[:, columns], preferred_element_type=jnp.float32), 0.0)
        hid[:, columns] = (lifted * lifted).astype(jnp.bfloat16)
    loop(0, W // tile, lift)

    def part_copy(d, block):
        target = (k + d) % K
        return pltpu.make_async_remote_copy(
            src_ref=stage.at[block, pl.ds(pl.multiple_of(target * tok, 16), tok)],
            dst_ref=part.at[d - 1, block],
            send_sem=part_send.at[d - 1, block], recv_sem=part_recv.at[d - 1, block],
            device_id=at_k(target), device_id_type=MESH)

    def lower(origin_a):
        def group(gi):
            settle(1, origin_a, gi)
            g = (gr + gi) % G
            block = origin_a * G + g
            rows = pl.ds(pl.multiple_of(g * (F * R) + origin_a * (2 * R), 2 * R), 2 * R)
            value = lax.dot_general(hid[...], down_full[rows, :], (((1,), (1,)), ((), ())),
                                    preferred_element_type=jnp.float32)
            stage[block] = value.astype(jnp.bfloat16)
            for d in range(1, K):
                part_copy(d, block).start()
        loop(0, G, group)

    def lower_ring(s):
        @pl.when(a - 1 - s >= 0)
        def _():
            lower(a - 1 - s)

        @pl.when(a + 1 + s < A)
        def _():
            lower(a + 1 + s)

    lower(a)
    loop(1, A - 1, lambda s: line(1, s, between=lambda: lower_ring(s - 1)))
    lower_ring(A - 2)

    for block in range(A * G):
        total = stage[block, mine].astype(jnp.float32)
        for d in range(1, K):
            there = part.at[d - 1, block]
            pltpu.make_async_copy(there, there, part_recv.at[d - 1, block]).wait()
            total += part[d - 1, block].astype(jnp.float32)
        begin = (block % G) * (F * R) + (block // G) * (2 * R)
        out_ref[:, begin:begin + 2 * R] = total.astype(jnp.bfloat16)

    def drain(block):
        for d in range(1, K):
            part_copy(d, block).wait_send()
    loop(0, A * G, drain)
    tokens(True)
    for m in range(2):
        for c in range(C):
            for b in range(G):
                hand(m, b, c, True)
        own(m, True)
        mated(m, True)
        loop(0, A - 1, lambda s: line(m, s, True))


def body(G, F, T, prompt_tokens, up_master, down_master, norm_gain):
    R, width = up_master.shape
    tok = prompt_tokens.shape[0]
    D, W = R * G * F, width // G
    A, K = F // 2, G * T
    C = R // min(CHUNK, R)
    NQ = G * C
    bf16 = jnp.bfloat16
    any_space = pl.BlockSpec(memory_space=pl.ANY)
    vmem_space = pl.BlockSpec(memory_space=pltpu.VMEM)
    dma = pltpu.SemaphoreType.DMA
    return pl.pallas_call(
        functools.partial(kernel, G, F, T),
        name="handoff",
        out_shape=(
            pltpu.MemorySpace.VMEM((D, W), bf16),
            pltpu.MemorySpace.VMEM((D, W), bf16),
            jax.ShapeDtypeStruct((tok, D), bf16),
        ),
        in_specs=[any_space, vmem_space, any_space, any_space],
        out_specs=(vmem_space,) * 3,
        scratch_shapes=[
            pltpu.VMEM((2, R, width), jnp.float32),
            pltpu.VMEM((2, R, width), bf16),
            pltpu.VMEM((tok, D), bf16),
            pltpu.VMEM((K * tok, D), bf16),
            pltpu.VMEM((K * tok, W), bf16),
            pltpu.VMEM((A * G, K * tok, 2 * R), bf16),
            pltpu.VMEM((K - 1, A * G, tok, 2 * R), bf16),
            dma((2, F, NQ)), dma((2, F, NQ)), dma((2, F, NQ)), dma((2, F, NQ)),
            dma((2, G, C)), dma((K - 1,)), dma((K - 1,)),
            dma((K - 1, A * G)), dma((K - 1, A * G)), dma((1,)), dma((2, C)),
        ],
        compiler_params=pltpu.CompilerParams(
            collective_id=0, has_side_effects=True, vmem_limit_bytes=43 * 1024 * 1024),
    )(prompt_tokens, norm_gain.reshape(1, R), up_master, down_master)


def solution(mesh):
    placed = (
        P(("gr", "fs", "tp"), None),
        P(("gr", "fs"), "tp"),
        P(("gr", "fs"), "tp"),
        P(("gr", "fs")),
    )
    return jax.shard_map(
        functools.partial(body, mesh.shape["gr"], mesh.shape["fs"], mesh.shape["tp"]),
        mesh=mesh,
        in_specs=placed,
        out_specs=(P(None, ("gr", "tp")), P(None, ("gr", "tp")), P(("gr", "fs", "tp"), None)),
        check_vma=False,
    )
```

```python
import functools

import jax
import jax.numpy as jnp
from jax import lax
from jax.experimental import pallas as pl
from jax.experimental.pallas import tpu as pltpu
from jax.sharding import PartitionSpec as P

MESH = pl.DeviceIdType.MESH
CHUNK = 16
TILE = 256
SPLIT = 4


def kernel(G, F, T, tok_in, gain_in, up_in, down_in, up_full, down_full, part,
           wide, narrow, raw, nrm, hid, stage,
           recv, sendl, sendr, sendy, send0, tok_recv, tok_send,
           part_recv, part_send, local_sem, load_sem):
    gr, f, tp = lax.axis_index("gr"), lax.axis_index("fs"), lax.axis_index("tp")
    full = (up_full, down_full)
    A = F // 2
    a, y = f // 2, f % 2
    mate = a * 2 + 1 - y
    R = up_in.shape[0]
    D, W = up_full.shape
    tok = tok_in.shape[0]
    CH = min(CHUNK, R)
    C = R // CH
    NQ = G * C
    PAIR_FIRST = (NQ * 5 // 32, (NQ * 5 + 31) // 32)
    K = G * T
    k = gr * T + tp
    weights = (up_in, down_in)

    def at_k(kk):
        return (kk // T, f, kk % T)

    def load(m, c):
        rows = pl.ds(c * CH, CH)
        return pltpu.make_async_copy(weights[m].at[rows], wide.at[m, rows], load_sem.at[m, c])

    token_load = pltpu.make_async_copy(tok_in, raw, local_sem.at[0])
    for c in range(C):
        load(0, c).start()
    token_load.start()
    for c in range(C):
        load(1, c).start()

    barrier = pltpu.get_barrier_semaphore()
    for d in range(1, K):
        pl.semaphore_signal(barrier, inc=1, device_id=at_k((k + d) % K), device_id_type=MESH)
    pl.semaphore_signal(barrier, inc=1, device_id=(gr, mate, tp), device_id_type=MESH)

    for shift in (1, A - 1):
        near = lax.rem(a + shift, A) * 2 + y
        pl.semaphore_signal(barrier, inc=1, device_id=(gr, near, tp), device_id_type=MESH)
    pl.semaphore_wait(barrier, K + 2)

    def rows_of(origin, g, c):
        return pl.ds(pl.multiple_of(g * (F * R) + origin * R + c * CH, CH), CH)

    home = k // G == tp

    def cast(m, c):
        rows = pl.ds(c * CH, CH)
        load(m, c).wait()
        value = wide[m, rows, :]
        if m == 0:
            value = value * column[c * CH:(c + 1) * CH]
        value = value.astype(jnp.bfloat16)
        narrow[m, rows, :] = value
        for b in range(G):
            @pl.when(tp * G + b == k)
            def _():
                full[m][rows_of(f, gr, c), :] = value[:, b * W:(b + 1) * W]

    def hand(m, b, c, wait):
        kk = tp * G + b
        q = ((gr - kk // T + G) % G) * C + c

        @pl.when(kk != k)
        def _():
            copy = pltpu.make_async_remote_copy(
                src_ref=narrow.at[m, pl.ds(c * CH, CH), pl.ds(b * W, W)],
                dst_ref=full[m].at[rows_of(f, gr, c)],
                send_sem=send0.at[m, b, c], recv_sem=recv.at[m, f, q],
                device_id=at_k(kk), device_id_type=MESH)
            if wait:
                copy.wait_send()
            else:
                copy.start()

    mine = pl.ds(pl.multiple_of(k * tok, 16), tok)

    def tokens(wait):
        for d in range(1, K):
            copy = pltpu.make_async_remote_copy(
                src_ref=nrm.at[mine], dst_ref=nrm.at[mine],
                send_sem=tok_send.at[d - 1], recv_sem=tok_recv.at[d - 1],
                device_id=at_k((k + d) % K), device_id_type=MESH)
            if wait:
                copy.wait_send()
            else:
                copy.start()

    def normalize(i, carry):
        values = raw[pl.ds(pl.multiple_of(i * 16, 16), 16), :].astype(jnp.float32)
        center = jnp.mean(values, axis=-1, keepdims=True)
        moved = values - center
        spread = jnp.mean(jnp.square(moved), axis=-1, keepdims=True)
        nrm[pl.ds(pl.multiple_of(k * tok + i * 16, 16), 16), :] = (
            moved * lax.rsqrt(spread + 1e-05)).astype(jnp.bfloat16)
        return carry

    rowed = lax.broadcasted_iota(jnp.int32, (R, R), 0) == lax.broadcasted_iota(jnp.int32, (R, R), 1)
    column = jnp.sum(jnp.where(rowed, gain_in[...], 0.0), axis=1, keepdims=True)

    cast(0, 0)
    for c in range(C):
        if c + 1 < C:
            cast(0, c + 1)
        else:
            cast(1, 0)
        for b in range(G):
            hand(0, b, c, False)

    def chunk(m, origin, q):
        return full[m].at[rows_of(origin, (gr + q // C) % G, q % C)]

    def send(m, origin, q, sems, target, wait):
        ref = chunk(m, origin, q)
        copy = pltpu.make_async_remote_copy(
            src_ref=ref, dst_ref=ref, send_sem=sems.at[m, origin, q], recv_sem=recv.at[m, origin, q],
            device_id=(gr, target, tp), device_id_type=MESH)
        if wait:
            copy.wait_send()
        else:
            copy.start()

    def arrived(m, origin, q):
        ref = chunk(m, origin, q)
        pltpu.make_async_copy(ref, ref, recv.at[m, origin, q]).wait()

    def left(m, origin, q, wait):
        @pl.when(a > 0)
        def _():
            send(m, origin, q, sendl, f - 2, wait)

    def right(m, origin, q, wait):
        @pl.when(a < A - 1)
        def _():
            send(m, origin, q, sendr, f + 2, wait)

    def loop(low, high, step):
        def go(i, carry):
            step(i)
            return carry
        if high > low:
            lax.fori_loop(low, high, go, 0)

    def own(m, wait=False):
        def step(q):
            if not wait:
                @pl.when(jnp.logical_or(q >= C, jnp.logical_not(home)))
                def _():
                    arrived(m, f, q)
            left(m, f, q, wait)
            right(m, f, q, wait)
            send(m, f, q, sendy, mate, wait)
        if m == 0:
            loop(0, NQ, step)
        else:
            loop(0, PAIR_FIRST[m], step)
            loop(C, NQ, step)
            loop(PAIR_FIRST[m], C, step)

    def mated(m, wait=False):
        def step(q):
            if not wait:
                arrived(m, mate, q)
            left(m, mate, q, wait)
            right(m, mate, q, wait)
        loop(0, PAIR_FIRST[m], step)

    def line(m, s, wait=False, between=None, eager=None):
        below, above = a - 1 - s, a + 1 + s

        def pass_on(origin_a, side, q, onward, across):
            origin = origin_a * 2 + side
            if not wait:
                arrived(m, origin, q)
            onward(m, origin, q, wait)
            if across:
                send(m, origin, q, sendy, mate, wait)

        def both(side, across):
            def step(q):
                @pl.when(below >= 0)
                def _():
                    pass_on(below, side, q, right, across)

                @pl.when(above < A)
                def _():
                    pass_on(above, side, q, left, across)
            return step

        pf = PAIR_FIRST[m]
        loop(0, pf, both(y, False))
        if m == 0:
            loop(pf, NQ, both(y, True))
        else:
            loop(C, NQ, both(y, True))
            if between is not None:
                between()
            loop(pf, C, both(y, True))
        if eager is not None:
            eager()
        loop(0, pf, both(1 - y, False))

    def settle(m, origin_a, gi):
        low = jnp.maximum(PAIR_FIRST[m], gi * C)

        def go(q, carry):
            arrived(m, origin_a * 2 + 1 - y, q)
            return carry
        lax.fori_loop(low, (gi + 1) * C, go, 0)

    def settle_all(i):
        for gi in range(G):
            settle(0, i, gi)

    own(0)
    token_load.wait()
    lax.fori_loop(0, tok // 16, normalize, 0)
    for c in range(C):
        if c + 1 < C:
            cast(1, c + 1)
        for b in range(G):
            hand(1, b, c, False)
    tokens(False)
    mated(0)
    loop(0, A - 2, lambda s: line(0, s))
    own(1)
    line(0, A - 2)
    mated(1)
    line(1, 0)

    loop(0, A, settle_all)
    for d in range(1, K):
        there = nrm.at[pl.ds(pl.multiple_of(((k - d + K) % K) * tok, 16), tok)]
        pltpu.make_async_copy(there, there, tok_recv.at[d - 1]).wait()

    tile = min(TILE, W)

    def lift(j):
        columns = pl.ds(pl.multiple_of(j * tile, tile), tile)
        lifted = jnp.maximum(jnp.dot(nrm[...], up_full[:, columns], preferred_element_type=jnp.float32), 0.0)
        hid[:, columns] = (lifted * lifted).astype(jnp.bfloat16)
    loop(0, W // tile, lift)

    def part_copy(d, block):
        target = (k + d) % K
        return pltpu.make_async_remote_copy(
            src_ref=stage.at[block, pl.ds(pl.multiple_of(target * tok, 16), tok)],
            dst_ref=part.at[d - 1, block],
            send_sem=part_send.at[d - 1, block], recv_sem=part_recv.at[d - 1, block],
            device_id=at_k(target), device_id_type=MESH)

    def lower(origin_a, gi):
        settle(1, origin_a, gi)
        g = (gr + gi) % G
        block = origin_a * G + g
        rows = pl.ds(pl.multiple_of(g * (F * R) + origin_a * (2 * R), 2 * R), 2 * R)
        value = lax.dot_general(hid[...], down_full[rows, :], (((1,), (1,)), ((), ())),
                                preferred_element_type=jnp.float32)
        stage[block] = value.astype(jnp.bfloat16)
        part[K - 1, block] = stage[block, mine]
        for d in range(1, K):
            part_copy(d, block).start()

    def lower_ring(s, low=0, high=G):
        @pl.when(a - 1 - s >= 0)
        def _():
            loop(low, high, lambda i: lower(a - 1 - s, G - 1 - i))

        @pl.when(a + 1 + s < A)
        def _():
            loop(low, high, lambda i: lower(a + 1 + s, G - 1 - i))

    loop(0, G, lambda i: lower(a, G - 1 - i))
    loop(1, A - 2, lambda s: line(1, s, between=lambda: lower_ring(s - 1)))
    line(1, A - 2, between=lambda: lower_ring(A - 3), eager=lambda: lower_ring(A - 2, 0, G - 1))
    lower_ring(A - 2, G - 1, G)

    for d in range(1, K):
        def landed(block):
            there = part.at[d - 1, block]
            pltpu.make_async_copy(there, there, part_recv.at[d - 1, block]).wait()
        loop(0, A * G, landed)

    def drain(block):
        for d in range(1, K):
            part_copy(d, block).wait_send()
    loop(0, A * G, drain)
    tokens(True)
    for m in range(2):
        for c in range(C):
            for b in range(G):
                hand(m, b, c, True)
        own(m, True)
        mated(m, True)
        loop(0, A - 1, lambda s: line(m, s, True))


def finish(G, F, up_held, down_held, parts, up_out, down_out, out_ref, sems):
    def out(m, i):
        source, target = ((up_held, up_out), (down_held, down_out))[m]
        size = source.shape[0] // SPLIT
        rows = pl.ds(i * size, size)
        return pltpu.make_async_copy(source.at[rows], target.at[rows], sems.at[m, i])

    for m in range(2):
        for i in range(SPLIT):
            out(m, i).start()
    K, blocks, _, wide = parts.shape
    D = out_ref.shape[1]
    for block in range(blocks):
        total = parts[0, block].astype(jnp.float32)
        for i in range(1, K):
            total += parts[i, block].astype(jnp.float32)
        begin = (block % G) * (D // G) + (block // G) * wide
        out_ref[:, begin:begin + wide] = total.astype(jnp.bfloat16)
    for m in range(2):
        for i in range(SPLIT):
            out(m, i).wait()


def body(G, F, T, prompt_tokens, up_master, down_master, norm_gain):
    R, width = up_master.shape
    tok = prompt_tokens.shape[0]
    D, W = R * G * F, width // G
    A, K = F // 2, G * T
    C = R // min(CHUNK, R)
    NQ = G * C
    bf16 = jnp.bfloat16
    any_space = pl.BlockSpec(memory_space=pl.ANY)
    vmem_space = pl.BlockSpec(memory_space=pltpu.VMEM)
    dma = pltpu.SemaphoreType.DMA
    up_held, down_held, parts = pl.pallas_call(
        functools.partial(kernel, G, F, T),
        name="handoff",
        out_shape=(
            pltpu.MemorySpace.VMEM((D, W), bf16),
            pltpu.MemorySpace.VMEM((D, W), bf16),
            pltpu.MemorySpace.VMEM((K, A * G, tok, 2 * R), bf16),
        ),
        in_specs=[any_space, vmem_space, any_space, any_space],
        out_specs=(vmem_space,) * 3,
        scratch_shapes=[
            pltpu.VMEM((2, R, width), jnp.float32),
            pltpu.VMEM((2, R, width), bf16),
            pltpu.VMEM((tok, D), bf16),
            pltpu.VMEM((K * tok, D), bf16),
            pltpu.VMEM((K * tok, W), bf16),
            pltpu.VMEM((A * G, K * tok, 2 * R), bf16),
            dma((2, F, NQ)), dma((2, F, NQ)), dma((2, F, NQ)), dma((2, F, NQ)),
            dma((2, G, C)), dma((K - 1,)), dma((K - 1,)),
            dma((K - 1, A * G)), dma((K - 1, A * G)), dma((1,)), dma((2, C)),
        ],
        compiler_params=pltpu.CompilerParams(
            collective_id=0, has_side_effects=True, vmem_limit_bytes=41 * 1024 * 1024),
    )(prompt_tokens, norm_gain.reshape(1, R), up_master, down_master)
    return pl.pallas_call(
        functools.partial(finish, G, F),
        name="finish",
        out_shape=(
            jax.ShapeDtypeStruct((D, W), bf16),
            jax.ShapeDtypeStruct((D, W), bf16),
            jax.ShapeDtypeStruct((tok, D), bf16),
        ),
        in_specs=[vmem_space] * 3,
        out_specs=(any_space, any_space, vmem_space),
        scratch_shapes=[dma((2, SPLIT))],
        compiler_params=pltpu.CompilerParams(vmem_limit_bytes=16 * 1024 * 1024),
    )(up_held, down_held, parts)


def solution(mesh):
    placed = (
        P(("gr", "fs", "tp"), None),
        P(("gr", "fs"), "tp"),
        P(("gr", "fs"), "tp"),
        P(("gr", "fs")),
    )
    return jax.shard_map(
        functools.partial(body, mesh.shape["gr"], mesh.shape["fs"], mesh.shape["tp"]),
        mesh=mesh,
        in_specs=placed,
        out_specs=(P(None, ("gr", "tp")), P(None, ("gr", "tp")), P(("gr", "fs", "tp"), None)),
        check_vma=False,
    )
```

```python
import functools

import jax
import jax.numpy as jnp
from jax import lax
from jax.experimental import pallas as pl
from jax.experimental.pallas import tpu as pltpu
from jax.sharding import PartitionSpec as P

MESH = pl.DeviceIdType.MESH
CHUNK = 32
TILE = 256
SPLIT = 4


def kernel(G, F, T, tok_in, gain_in, up_in, down_in, up_full, down_full, part,
           wide, narrow, raw, nrm, hid, stage,
           recv, sendl, sendr, sendy, send0, tok_recv, tok_send,
           part_recv, part_send, local_sem, load_sem):
    gr, f, tp = lax.axis_index("gr"), lax.axis_index("fs"), lax.axis_index("tp")
    full = (up_full, down_full)
    A = F // 2
    a, y = f // 2, f % 2
    mate = a * 2 + 1 - y
    R = up_in.shape[0]
    D, W = up_full.shape
    tok = tok_in.shape[0]
    CH = min(CHUNK, R)
    C = R // CH
    NQ = G * C
    PAIR_FIRST = (NQ * 5 // 32, (NQ * 5 + 31) // 32)
    K = G * T
    k = gr * T + tp
    weights = (up_in, down_in)

    def at_k(kk):
        return (kk // T, f, kk % T)

    def load(m, c):
        rows = pl.ds(c * CH, CH)
        return pltpu.make_async_copy(weights[m].at[rows], wide.at[m, rows], load_sem.at[m, c])

    token_load = pltpu.make_async_copy(tok_in, raw, local_sem.at[0])
    for c in range(C):
        load(0, c).start()
    token_load.start()
    for c in range(C):
        load(1, c).start()

    barrier = pltpu.get_barrier_semaphore()
    for d in range(1, K):
        pl.semaphore_signal(barrier, inc=1, device_id=at_k((k + d) % K), device_id_type=MESH)
    pl.semaphore_signal(barrier, inc=1, device_id=(gr, mate, tp), device_id_type=MESH)

    for shift in (1, A - 1):
        near = lax.rem(a + shift, A) * 2 + y
        pl.semaphore_signal(barrier, inc=1, device_id=(gr, near, tp), device_id_type=MESH)
    pl.semaphore_wait(barrier, K + 2)

    def rows_of(origin, g, c):
        return pl.ds(pl.multiple_of(g * (F * R) + origin * R + c * CH, CH), CH)

    home = k // G == tp

    def cast(m, c):
        rows = pl.ds(c * CH, CH)
        load(m, c).wait()
        value = wide[m, rows, :]
        if m == 0:
            value = value * column[c * CH:(c + 1) * CH]
        value = value.astype(jnp.bfloat16)
        narrow[m, rows, :] = value
        for b in range(G):
            @pl.when(tp * G + b == k)
            def _():
                full[m][rows_of(f, gr, c), :] = value[:, b * W:(b + 1) * W]

    def hand(m, b, c, wait):
        kk = tp * G + b
        q = ((gr - kk // T + G) % G) * C + c

        @pl.when(kk != k)
        def _():
            copy = pltpu.make_async_remote_copy(
                src_ref=narrow.at[m, pl.ds(c * CH, CH), pl.ds(b * W, W)],
                dst_ref=full[m].at[rows_of(f, gr, c)],
                send_sem=send0.at[m, b, c], recv_sem=recv.at[m, f, q],
                device_id=at_k(kk), device_id_type=MESH)
            if wait:
                copy.wait_send()
            else:
                copy.start()

    mine = pl.ds(pl.multiple_of(k * tok, 16), tok)

    def tokens(wait):
        for d in range(1, K):
            copy = pltpu.make_async_remote_copy(
                src_ref=nrm.at[mine], dst_ref=nrm.at[mine],
                send_sem=tok_send.at[d - 1], recv_sem=tok_recv.at[d - 1],
                device_id=at_k((k + d) % K), device_id_type=MESH)
            if wait:
                copy.wait_send()
            else:
                copy.start()

    def normalize(i, carry):
        values = raw[pl.ds(pl.multiple_of(i * 16, 16), 16), :].astype(jnp.float32)
        center = jnp.mean(values, axis=-1, keepdims=True)
        moved = values - center
        spread = jnp.mean(jnp.square(moved), axis=-1, keepdims=True)
        nrm[pl.ds(pl.multiple_of(k * tok + i * 16, 16), 16), :] = (
            moved * lax.rsqrt(spread + 1e-05)).astype(jnp.bfloat16)
        return carry

    rowed = lax.broadcasted_iota(jnp.int32, (R, R), 0) == lax.broadcasted_iota(jnp.int32, (R, R), 1)
    column = jnp.sum(jnp.where(rowed, gain_in[...], 0.0), axis=1, keepdims=True)

    cast(0, 0)
    for c in range(C):
        if c + 1 < C:
            cast(0, c + 1)
        else:
            cast(1, 0)
        for b in range(G):
            hand(0, b, c, False)

    def chunk(m, origin, q):
        return full[m].at[rows_of(origin, (gr + q // C) % G, q % C)]

    def send(m, origin, q, sems, target, wait):
        ref = chunk(m, origin, q)
        copy = pltpu.make_async_remote_copy(
            src_ref=ref, dst_ref=ref, send_sem=sems.at[m, origin, q], recv_sem=recv.at[m, origin, q],
            device_id=(gr, target, tp), device_id_type=MESH)
        if wait:
            copy.wait_send()
        else:
            copy.start()

    def arrived(m, origin, q):
        ref = chunk(m, origin, q)
        pltpu.make_async_copy(ref, ref, recv.at[m, origin, q]).wait()

    def left(m, origin, q, wait):
        @pl.when(a > 0)
        def _():
            send(m, origin, q, sendl, f - 2, wait)

    def right(m, origin, q, wait):
        @pl.when(a < A - 1)
        def _():
            send(m, origin, q, sendr, f + 2, wait)

    def loop(low, high, step):
        def go(i, carry):
            step(i)
            return carry
        if high > low:
            lax.fori_loop(low, high, go, 0)

    def own(m, wait=False):
        def step(q):
            if not wait:
                @pl.when(jnp.logical_or(q >= C, jnp.logical_not(home)))
                def _():
                    arrived(m, f, q)
            left(m, f, q, wait)
            right(m, f, q, wait)
            send(m, f, q, sendy, mate, wait)
        if m == 0:
            loop(0, NQ, step)
        else:
            loop(0, PAIR_FIRST[m], step)
            loop(C, NQ, step)
            loop(PAIR_FIRST[m], C, step)

    def mated(m, wait=False):
        def step(q):
            if not wait:
                arrived(m, mate, q)
            left(m, mate, q, wait)
            right(m, mate, q, wait)
        loop(0, PAIR_FIRST[m], step)

    def line(m, s, wait=False, between=None, eager=None):
        below, above = a - 1 - s, a + 1 + s

        def pass_on(origin_a, side, q, onward, across):
            origin = origin_a * 2 + side
            if not wait:
                arrived(m, origin, q)
            onward(m, origin, q, wait)
            if across:
                send(m, origin, q, sendy, mate, wait)

        def both(side, across):
            def step(q):
                @pl.when(below >= 0)
                def _():
                    pass_on(below, side, q, right, across)

                @pl.when(above < A)
                def _():
                    pass_on(above, side, q, left, across)
            return step

        pf = PAIR_FIRST[m]
        loop(0, pf, both(y, False))
        if m == 0:
            loop(pf, NQ, both(y, True))
        else:
            loop(C, NQ, both(y, True))
            if between is not None:
                between()
            loop(pf, C, both(y, True))
        if eager is not None:
            eager()
        loop(0, pf, both(1 - y, False))

    def settle(m, origin_a, gi):
        low = jnp.maximum(PAIR_FIRST[m], gi * C)

        def go(q, carry):
            arrived(m, origin_a * 2 + 1 - y, q)
            return carry
        lax.fori_loop(low, (gi + 1) * C, go, 0)

    def settle_all(i):
        for gi in range(G):
            settle(0, i, gi)

    own(0)
    token_load.wait()
    lax.fori_loop(0, tok // 16, normalize, 0)
    for c in range(C):
        if c + 1 < C:
            cast(1, c + 1)
        for b in range(G):
            hand(1, b, c, False)
    tokens(False)
    mated(0)
    loop(0, A - 2, lambda s: line(0, s))
    own(1)
    line(0, A - 2)
    mated(1)
    line(1, 0)

    loop(0, A, settle_all)
    for d in range(1, K):
        there = nrm.at[pl.ds(pl.multiple_of(((k - d + K) % K) * tok, 16), tok)]
        pltpu.make_async_copy(there, there, tok_recv.at[d - 1]).wait()

    tile = min(TILE, W)

    def lift(j):
        columns = pl.ds(pl.multiple_of(j * tile, tile), tile)
        lifted = jnp.maximum(jnp.dot(nrm[...], up_full[:, columns], preferred_element_type=jnp.float32), 0.0)
        hid[:, columns] = (lifted * lifted).astype(jnp.bfloat16)
    loop(0, W // tile, lift)

    def part_copy(d, block):
        target = (k + d) % K
        return pltpu.make_async_remote_copy(
            src_ref=stage.at[block, pl.ds(pl.multiple_of(target * tok, 16), tok)],
            dst_ref=part.at[d - 1, block],
            send_sem=part_send.at[d - 1, block], recv_sem=part_recv.at[d - 1, block],
            device_id=at_k(target), device_id_type=MESH)

    def lower(origin_a, gi):
        settle(1, origin_a, gi)
        g = (gr + gi) % G
        block = origin_a * G + g
        rows = pl.ds(pl.multiple_of(g * (F * R) + origin_a * (2 * R), 2 * R), 2 * R)
        value = lax.dot_general(hid[...], down_full[rows, :], (((1,), (1,)), ((), ())),
                                preferred_element_type=jnp.float32)
        stage[block] = value.astype(jnp.bfloat16)
        part[K - 1, block] = stage[block, mine]
        for d in range(1, K):
            part_copy(d, block).start()

    def lower_ring(s, low=0, high=G):
        @pl.when(a - 1 - s >= 0)
        def _():
            loop(low, high, lambda i: lower(a - 1 - s, G - 1 - i))

        @pl.when(a + 1 + s < A)
        def _():
            loop(low, high, lambda i: lower(a + 1 + s, G - 1 - i))

    loop(0, G, lambda i: lower(a, G - 1 - i))
    loop(1, A - 2, lambda s: line(1, s, between=lambda: lower_ring(s - 1)))
    line(1, A - 2, between=lambda: lower_ring(A - 3), eager=lambda: lower_ring(A - 2, 0, G - 1))
    lower_ring(A - 2, G - 1, G)

    for d in range(1, K):
        def landed(block):
            there = part.at[d - 1, block]
            pltpu.make_async_copy(there, there, part_recv.at[d - 1, block]).wait()
        loop(0, A * G, landed)

    def drain(block):
        for d in range(1, K):
            part_copy(d, block).wait_send()
    loop(0, A * G, drain)
    tokens(True)
    for m in range(2):
        for c in range(C):
            for b in range(G):
                hand(m, b, c, True)
        own(m, True)
        mated(m, True)
        loop(0, A - 1, lambda s: line(m, s, True))


def finish(G, F, up_held, down_held, parts, up_out, down_out, out_ref, sems):
    def out(m, i):
        source, target = ((up_held, up_out), (down_held, down_out))[m]
        size = source.shape[0] // SPLIT
        rows = pl.ds(i * size, size)
        return pltpu.make_async_copy(source.at[rows], target.at[rows], sems.at[m, i])

    for m in range(2):
        for i in range(SPLIT):
            out(m, i).start()
    K, blocks, _, wide = parts.shape
    D = out_ref.shape[1]
    for block in range(blocks):
        total = parts[0, block].astype(jnp.float32)
        for i in range(1, K):
            total += parts[i, block].astype(jnp.float32)
        begin = (block % G) * (D // G) + (block // G) * wide
        out_ref[:, begin:begin + wide] = total.astype(jnp.bfloat16)
    for m in range(2):
        for i in range(SPLIT):
            out(m, i).wait()


def body(G, F, T, prompt_tokens, up_master, down_master, norm_gain):
    R, width = up_master.shape
    tok = prompt_tokens.shape[0]
    D, W = R * G * F, width // G
    A, K = F // 2, G * T
    C = R // min(CHUNK, R)
    NQ = G * C
    bf16 = jnp.bfloat16
    any_space = pl.BlockSpec(memory_space=pl.ANY)
    vmem_space = pl.BlockSpec(memory_space=pltpu.VMEM)
    dma = pltpu.SemaphoreType.DMA
    up_held, down_held, parts = pl.pallas_call(
        functools.partial(kernel, G, F, T),
        name="handoff",
        out_shape=(
            pltpu.MemorySpace.VMEM((D, W), bf16),
            pltpu.MemorySpace.VMEM((D, W), bf16),
            pltpu.MemorySpace.VMEM((K, A * G, tok, 2 * R), bf16),
        ),
        in_specs=[any_space, vmem_space, any_space, any_space],
        out_specs=(vmem_space,) * 3,
        scratch_shapes=[
            pltpu.VMEM((2, R, width), jnp.float32),
            pltpu.VMEM((2, R, width), bf16),
            pltpu.VMEM((tok, D), bf16),
            pltpu.VMEM((K * tok, D), bf16),
            pltpu.VMEM((K * tok, W), bf16),
            pltpu.VMEM((A * G, K * tok, 2 * R), bf16),
            dma((2, F, NQ)), dma((2, F, NQ)), dma((2, F, NQ)), dma((2, F, NQ)),
            dma((2, G, C)), dma((K - 1,)), dma((K - 1,)),
            dma((K - 1, A * G)), dma((K - 1, A * G)), dma((1,)), dma((2, C)),
        ],
        compiler_params=pltpu.CompilerParams(
            collective_id=0, has_side_effects=True, vmem_limit_bytes=41 * 1024 * 1024),
    )(prompt_tokens, norm_gain.reshape(1, R), up_master, down_master)
    return pl.pallas_call(
        functools.partial(finish, G, F),
        name="finish",
        out_shape=(
            jax.ShapeDtypeStruct((D, W), bf16),
            jax.ShapeDtypeStruct((D, W), bf16),
            jax.ShapeDtypeStruct((tok, D), bf16),
        ),
        in_specs=[vmem_space] * 3,
        out_specs=(any_space, any_space, vmem_space),
        scratch_shapes=[dma((2, SPLIT))],
        compiler_params=pltpu.CompilerParams(vmem_limit_bytes=16 * 1024 * 1024),
    )(up_held, down_held, parts)


def solution(mesh):
    placed = (
        P(("gr", "fs", "tp"), None),
        P(("gr", "fs"), "tp"),
        P(("gr", "fs"), "tp"),
        P(("gr", "fs")),
    )
    return jax.shard_map(
        functools.partial(body, mesh.shape["gr"], mesh.shape["fs"], mesh.shape["tp"]),
        mesh=mesh,
        in_specs=placed,
        out_specs=(P(None, ("gr", "tp")), P(None, ("gr", "tp")), P(("gr", "fs", "tp"), None)),
        check_vma=False,
    )
```
